32 devices in a mesh: fs: 4 (over z), tp: 8 (over y, x, core).
Axes of the slice: x: 2, y: 2, z: 4, core: 2. Of those that a mesh axis runs over, the one named last changes fastest.
Arguments:
- saved_input: bfloat16 [4096, 2304], P('fs', 'tp'), may hold values from -6 to 6
- cot_forget: bfloat16 [4096, 2304], P('fs', 'tp'), may hold values from -0.09375 to 0.09375
- cot_value: bfloat16 [4096, 2304], P('fs', 'tp'), may hold values from -0.09375 to 0.09375
- basis_forget: bfloat16 [2304, 288], replicated, may hold values from -2 to 2
- basis_value: bfloat16 [2304, 288], replicated, may hold values from -2 to 2
- first_forget: float32 [288, 2304], P('fs', 'tp'), may hold values from -180 to 180
- first_value: float32 [288, 2304], P('fs', 'tp'), may hold values from -180 to 180
- second_forget: float32 [288, 2304], P('fs', 'tp'), may hold values from 0.1 to 1
- second_value: float32 [288, 2304], P('fs', 'tp'), may hold values from 0.1 to 1
- weight_forget: float32 [2304, 2304], P('fs', 'tp'), may hold values from -0.125 to 0.125
- weight_value: float32 [2304, 2304], P('fs', 'tp'), may hold values from -0.125 to 0.125
Outputs:
- new_first_forget: float32 [288, 2304], P('fs', 'tp')
- new_second_forget: float32 [288, 2304], P('fs', 'tp')
- step_forget: float32 [2304, 2304], P('fs', 'tp')
- new_weight_forget: float32 [2304, 2304], P('fs', 'tp')
- copy_forget: bfloat16 [2304, 2304], P(None, 'tp')
- new_first_value: float32 [288, 2304], P('fs', 'tp')
- new_second_value: float32 [288, 2304], P('fs', 'tp')
- step_value: float32 [2304, 2304], P('fs', 'tp')
- new_weight_value: float32 [2304, 2304], P('fs', 'tp')
- copy_value: bfloat16 [2304, 2304], P(None, 'tp')
The draws below stay inside these ranges and needn't reach their ends.
All inputs are finite; a program needn't handle non-finite values.
Results may differ from the reference program's by a relative error of at most 0.0042.
Values may be sent and summed in bfloat16 or wider, within the bound.
A program may use at most 64 MiB of HBM per device.

```python
import math
import jax
import jax.numpy as jnp
from jax import lax

D = 2304
RANK = 288
TOKENS = 4096


def rising_draw(key, row_count, col_count, col_span):
    raw_values = jnp.clip(jax.random.normal(key, (row_count, col_count), jnp.float32), -4.0, 4.0)
    stretch = math.log(3.0)
    row_pos = jnp.arange(row_count, dtype=jnp.float32) / max(row_count - 1, 1)
    col_pos = jnp.arange(col_count, dtype=jnp.float32) / max(col_count - 1, 1)
    factor = jnp.exp(stretch * (row_pos[:, None] + col_span * col_pos[None, :]))
    return raw_values * factor


def draw_basis_forget(key, part):
    return (rising_draw(jax.random.fold_in(key, 11), D, RANK, 0.0) * D ** (-0.5)).astype(jnp.bfloat16)


def draw_basis_value(key, part):
    return (rising_draw(jax.random.fold_in(key, 12), D, RANK, 0.0) * D ** (-0.5)).astype(jnp.bfloat16)


def draw_first_forget(key, part):
    return rising_draw(jax.random.fold_in(key, 13), RANK, D, 1.0)


def draw_first_value(key, part):
    return rising_draw(jax.random.fold_in(key, 14), RANK, D, 1.0)


def levels(own_key, dims, split, least, largest):
    loudness = 1.0
    for position, blocks in split:
        draws = jax.random.uniform(jax.random.fold_in(jax.random.fold_in(own_key, 6), position), (blocks,), jnp.float32, least / len(split), largest / len(split))
        loudness = loudness * jnp.repeat(jnp.exp(draws), dims[position] // blocks).reshape((-1,) + (1,) * (len(dims) - 1 - position))
    return loudness


def centred(rng, extent, scale, reach, shards=(), kind=jnp.bfloat16):
    entries = scale * jax.random.normal(rng, extent, jnp.float32)
    if shards:
        entries = entries * levels(rng, extent, shards, -0.22, 0.18)
    return jnp.clip(entries, -reach, reach).astype(kind)


def setup_inputs(seed: int = 0) -> dict:
    keys = jax.random.split(jax.random.key(seed), 12)
    return {
        "saved_input": centred(keys[0], (TOKENS, D), 1.0, 6.0, ((0, 4), (1, 8))),
        "cot_forget": centred(keys[1], (TOKENS, D), (TOKENS ** -0.5), 0.09375, ((0, 4), (1, 8))),
        "cot_value": centred(keys[2], (TOKENS, D), (TOKENS ** -0.5), 0.09375, ((0, 4), (1, 8))),
        "basis_forget": draw_basis_forget(jax.random.fold_in(keys[11], 71), 0),
        "basis_value": draw_basis_value(jax.random.fold_in(keys[11], 71), 0),
        "first_forget": draw_first_forget(jax.random.fold_in(keys[11], 71), 0),
        "first_value": draw_first_value(jax.random.fold_in(keys[11], 71), 0),
        "second_forget": jnp.clip(jnp.exp(math.log(1.0) - 2.3025851 * jax.random.uniform(keys[7], (RANK, D), jnp.float32) ** levels(keys[7], (RANK, D), ((0, 4), (1, 8)), -0.2, 0.2)), 0.1, 1.0),
        "second_value": jnp.clip(jnp.exp(math.log(1.0) - 2.3025851 * jax.random.uniform(keys[8], (RANK, D), jnp.float32) ** levels(keys[8], (RANK, D), ((0, 4), (1, 8)), -0.2, 0.2)), 0.1, 1.0),
        "weight_forget": centred(keys[9], (D, D), D ** -0.5, 0.125, ((0, 4), (1, 8)), jnp.float32),
        "weight_value": centred(keys[10], (D, D), D ** -0.5, 0.125, ((0, 4), (1, 8)), jnp.float32),
    }


beta_one = 0.8
beta_two = 0.9
rate = 0.02
epsilon = 1e-06

def project(saved_input, cotangent, basis):
    inputs_basis = jnp.dot(saved_input.astype(jnp.float32), basis.astype(jnp.float32), precision=lax.Precision.HIGHEST)
    return jnp.dot(inputs_basis.T, cotangent.astype(jnp.float32), precision=lax.Precision.HIGHEST)

def advance(projected, first, second, basis, weight):
    new_first = beta_one * first + (1.0 - beta_one) * projected
    new_second = beta_two * second + (1.0 - beta_two) * projected * projected
    direction = (new_first / jnp.sqrt(new_second)).astype(jnp.bfloat16)
    update = jnp.dot(basis.astype(jnp.float32), direction.astype(jnp.float32), precision=lax.Precision.HIGHEST)
    mean_square = jnp.mean(update * update)
    step = update / jnp.sqrt(mean_square + epsilon)
    new_weight = weight - rate * step
    return (new_first, new_second, step, new_weight, new_weight.astype(jnp.bfloat16))

def reference(saved_input, cot_forget, cot_value, basis_forget, basis_value, first_forget, first_value, second_forget, second_value, weight_forget, weight_value):
    proj_forget = project(saved_input, cot_forget, basis_forget)
    proj_value = project(saved_input, cot_value, basis_value)
    out_forget = advance(proj_forget, first_forget, second_forget, basis_forget, weight_forget)
    out_value = advance(proj_value, first_value, second_value, basis_value, weight_value)
    return (out_forget[0], out_forget[1], out_forget[2], out_forget[3], out_forget[4], out_value[0], out_value[1], out_value[2], out_value[3], out_value[4])
```

```python
import functools

import jax
import jax.numpy as jnp
from jax import lax
from jax.experimental import pallas as pl
from jax.experimental.pallas import tpu as pltpu
from jax.sharding import PartitionSpec as P

MESH = pl.DeviceIdType.MESH
LANES = 128

beta_one = 0.8
beta_two = 0.9
rate = 0.02
epsilon = 1e-06


def contract(left_part, right_part):
    return lax.dot_general(
        left_part,
        right_part,
        (((0,), (0,)), ((), ())),
        precision=lax.Precision.HIGHEST,
        preferred_element_type=jnp.float32,
    )


def moments(projected, first, second):
    new_first = beta_one * first + (1.0 - beta_one) * projected
    new_second = beta_two * second + (1.0 - beta_two) * projected * projected
    direction = (new_first / jnp.sqrt(new_second)).astype(jnp.bfloat16)
    return (new_first, new_second, direction)


def body(
    saved_input,
    cot_forget,
    cot_value,
    basis_forget,
    basis_value,
    first_forget,
    first_value,
    second_forget,
    second_value,
    weight_forget,
    weight_value,
):
    col_width = cot_forget.shape[1]
    own_rows = weight_forget.shape[0]
    col_first = lax.axis_index("tp") * col_width
    row_start = lax.axis_index("fs") * own_rows
    rows_forget = lax.dynamic_slice_in_dim(basis_forget, row_start, own_rows, 0)
    rows_value = lax.dynamic_slice_in_dim(basis_value, row_start, own_rows, 0)
    both_cots = jnp.concatenate([cot_forget, cot_value], axis=1)
    cols_forget = lax.dynamic_slice_in_dim(basis_forget, col_first, col_width, 0)
    cols_value = lax.dynamic_slice_in_dim(basis_value, col_first, col_width, 0)
    partial_forget = jnp.dot(saved_input, cols_forget, preferred_element_type=jnp.float32)
    partial_value = jnp.dot(saved_input, cols_value, preferred_element_type=jnp.float32)
    summed_forget, summed_value = lax.psum((partial_forget, partial_value), "tp")
    cots_wide = both_cots.astype(jnp.float32)
    projected = lax.psum_scatter(
        jnp.concatenate(
            [
                contract(summed_forget, cots_wide[:, :col_width]),
                contract(summed_value, cots_wide[:, col_width:]),
            ],
            axis=1,
        ),
        "fs",
        scatter_dimension=0,
        tiled=True,
    )
    new_first_forget, new_second_forget, direction_forget = moments(
        projected[:, :col_width], first_forget, second_forget
    )
    new_first_value, new_second_value, direction_value = moments(
        projected[:, col_width:], first_value, second_value
    )
    update_forget = jnp.dot(
        rows_forget,
        lax.all_gather(direction_forget, "fs", axis=0, tiled=True),
        preferred_element_type=jnp.float32,
    )
    update_value = jnp.dot(
        rows_value,
        lax.all_gather(direction_value, "fs", axis=0, tiled=True),
        preferred_element_type=jnp.float32,
    )
    square_forget, square_value = lax.psum(
        (jnp.sum(update_forget * update_forget), jnp.sum(update_value * update_value)), ("fs", "tp")
    )
    entries = float(basis_forget.shape[0] * weight_forget.shape[1] * lax.axis_size("tp"))
    step_forget = update_forget / jnp.sqrt(square_forget / entries + epsilon)
    step_value = update_value / jnp.sqrt(square_value / entries + epsilon)
    new_weight_forget = weight_forget - rate * step_forget
    new_weight_value = weight_value - rate * step_value
    copy_forget, copy_value = (
        lax.all_gather(new_weight_forget.astype(jnp.bfloat16), "fs", axis=0, tiled=True),
        lax.all_gather(new_weight_value.astype(jnp.bfloat16), "fs", axis=0, tiled=True),
    )
    return (
        new_first_forget,
        new_second_forget,
        step_forget,
        new_weight_forget,
        copy_forget,
        new_first_value,
        new_second_value,
        step_value,
        new_weight_value,
        copy_value,
    )


def pack(weights, odd, half):
    deep = weights[0].shape[0] // 2
    cols = weights[0].shape[1]
    side = LANES // 2
    whole = cols - side
    tiles = []
    rests = []
    for weight in weights:
        rows = weight[deep * half : deep * (half + 1)]
        kept = jnp.where(odd, rows[:, side:], rows[:, :whole])
        tiles += [kept[:, at : at + LANES] for at in range(0, whole, LANES)]
        rests.append(jnp.where(odd, rows[:, :side], rows[:, whole:]))
    rest = jnp.where(
        odd,
        jnp.concatenate([rests[1], rests[0]], axis=1),
        jnp.concatenate(rests, axis=1),
    )
    return jnp.stack(tiles + [rest]).astype(jnp.bfloat16)


def new_moments(projected, first, second):
    new_first = beta_one * first + (1.0 - beta_one) * projected
    new_second = beta_two * second + (1.0 - beta_two) * projected * projected
    return new_first, new_second


def contract_tokens(left, right):
    return lax.dot_general(
        left, right, (((1,), (1,)), ((), ())), preferred_element_type=jnp.float32
    )


def exchange(
    F, T,
    s_hbm, cf_hbm, cv_hbm, bf_hbm, bv_hbm, ff_hbm, fv_hbm, sf_hbm, sv_hbm, wf_hbm, wv_hbm,
    pr_out, d_out, ss_out, wg_out,
    s, c, b, fm, sm, w, sg, z, zg, psend, prx, pr, dg, d, ss, wg,
    in_sem, sg_own, sg_send, sg_recv, z_send, z_recv, zf_send, zf_recv,
    p_send, p_recv, d_send, d_recv, n_send, n_recv, w_send, w_recv, wl_send, wl_recv, out_sem, wo_sem,
):
    f = lax.axis_index("fs")
    t = lax.axis_index("tp")
    ranks = psend.shape[1] // 2
    block = zg.shape[3]
    right = lax.rem(f + 1, F)
    left = lax.rem(f + F - 1, F)
    far = lax.rem(f + 2, F)
    pair = t + 1 - 2 * lax.rem(t, 2)

    def tp_at(k):
        return lax.rem(t + k + T, T)

    def fs_at(k):
        return lax.rem(f + k + F, F)

    def tokens(k):
        return pl.ds(pl.multiple_of(k * block, block), block)

    def fetch(src, dst, sem):
        copy = pltpu.make_async_copy(src, dst, sem)
        copy.start()
        return copy

    def push(src, dst, send, recv, where):
        return pltpu.make_async_remote_copy(
            src_ref=src, dst_ref=dst, send_sem=send, recv_sem=recv,
            device_id=where, device_id_type=MESH,
        )

    load_w = [fetch(wf_hbm, w.at[0], in_sem.at[0]), fetch(wv_hbm, w.at[1], in_sem.at[1])]
    load_s = fetch(s_hbm, s, in_sem.at[2])
    load_own = fetch(s_hbm.at[:, tokens(t)], sg.at[t], sg_own)
    load_b = [fetch(bf_hbm, b.at[0], in_sem.at[3]), fetch(bv_hbm, b.at[1], in_sem.at[4])]
    load_c = [fetch(cf_hbm, c.at[0], in_sem.at[5]), fetch(cv_hbm, c.at[1], in_sem.at[6])]
    load_m = [
        fetch(ff_hbm, fm.at[0], in_sem.at[7]), fetch(fv_hbm, fm.at[1], in_sem.at[8]),
        fetch(sf_hbm, sm.at[0], in_sem.at[9]), fetch(sv_hbm, sm.at[1], in_sem.at[10]),
    ]

    barrier = pltpu.get_barrier_semaphore()
    for k in range(1, T):
        pl.semaphore_signal(barrier, inc=1, device_id={"tp": tp_at(k)}, device_id_type=MESH)
    for k in range(1, F):
        pl.semaphore_signal(barrier, inc=1, device_id={"fs": fs_at(k)}, device_id_type=MESH)
    for p in range(2):
        load_w[p].wait()
    both = [w[0], w[1]]
    for half in range(2):
        wg[f, half] = pack(both, lax.rem(f, 2) == 1, half)
    load_s.wait()
    pl.semaphore_wait(barrier, T + F - 2)

    sends = []
    for k in range(1, T):
        copy = push(s.at[:, tokens(tp_at(k))], sg.at[t], sg_send.at[k], sg_recv.at[k], {"tp": tp_at(k)})
        copy.start()
        sends.append(copy)
    own_right = [push(wg.at[f, p], wg.at[f, p], w_send.at[p], w_recv.at[p], {"fs": right}) for p in range(2)]
    own_left = [push(wg.at[f, p], wg.at[f, p], wl_send.at[p], wl_recv.at[p], {"fs": left}) for p in range(2)]
    own_right[0].start()
    own_left[1].start()
    own_right[1].start()
    own_left[0].start()
    sends += own_right + own_left

    load_own.wait()
    for copy in load_b:
        copy.wait()
    for k in range(1, T):
        source = tp_at(-k)
        push(s.at[:, tokens(t)], sg.at[source], sg_send.at[k], sg_recv.at[k], {"tp": source}).wait_recv()
    inputs = sg[...].reshape(b.shape[2], block)
    for p in range(2):
        z[p] = jnp.dot(b[p], inputs, preferred_element_type=jnp.float32).astype(jnp.bfloat16)

    chips = T // 2
    to_pair = push(z, zg.at[t], zf_send.at[0], zf_recv.at[0], {"tp": pair})
    for k in range(1, chips):
        copy = push(z, zg.at[t], z_send.at[k], z_recv.at[k], {"tp": tp_at(2 * k)})
        copy.start()
        sends.append(copy)
    to_pair.start()
    sends.append(to_pair)

    for copy in load_c:
        copy.wait()
    partial = [contract_tokens(z[p], c[p, :, tokens(t)]) for p in range(2)]

    def add(partial, source):
        return [
            partial[p] + contract_tokens(zg[source, p], c[p, :, tokens(source)])
            for p in range(2)
        ]

    push(z, zg.at[pair], zf_send.at[0], zf_recv.at[0], {"tp": pair}).wait_recv()
    partial = add(partial, pair)
    for k in range(1, chips):
        source = tp_at(-2 * k)
        push(z, zg.at[source], z_send.at[k], z_recv.at[k], {"tp": source}).wait_recv()
        copy = push(zg.at[source], zg.at[source], zf_send.at[k], zf_recv.at[k], {"tp": pair})
        copy.start()
        sends.append(copy)
        partial = add(partial, source)
    for k in range(1, chips):
        source = lax.rem(pair - 2 * k + T, T)
        push(z, zg.at[source], zf_send.at[k], zf_recv.at[k], {"tp": pair}).wait_recv()
        partial = add(partial, source)

    for q in range(F):
        rows = jnp.concatenate([part[q * ranks : (q + 1) * ranks] for part in partial], axis=0)
        psend[q] = rows.astype(jnp.bfloat16)
        own = jnp.where(f == q, rows, 0.0)
        total = own if q == 0 else total + own
    for k in (1, F - 1, *range(2, F - 1)):
        copy = push(psend.at[fs_at(k)], prx.at[f], p_send.at[k], p_recv.at[k], {"fs": fs_at(k)})
        copy.start()
        sends.append(copy)

    push(wg.at[f, 0], wg.at[left, 0], w_send.at[0], w_recv.at[0], {"fs": left}).wait_recv()
    on_right = push(wg.at[left, 0], wg.at[left, 0], w_send.at[2], w_recv.at[2], {"fs": right})
    on_right.start()
    push(wg.at[f, 1], wg.at[right, 1], wl_send.at[1], wl_recv.at[1], {"fs": right}).wait_recv()
    on_left = push(wg.at[right, 1], wg.at[right, 1], wl_send.at[2], wl_recv.at[2], {"fs": left})
    on_left.start()
    sends += [on_right, on_left]

    for copy in load_m:
        copy.wait()
    for k in (1, F - 1, *range(2, F - 1)):
        push(psend.at[f], prx.at[fs_at(-k)], p_send.at[k], p_recv.at[k], {"fs": fs_at(-k)}).wait_recv()
    for k in range(1, F):
        total = total + prx[fs_at(-k)].astype(jnp.float32)
    pr[...] = total
    new_first, new_second = new_moments(total, fm[...].reshape(total.shape), sm[...].reshape(total.shape))
    dg[f] = (new_first / jnp.sqrt(new_second)).astype(jnp.bfloat16)
    outs = [fetch(pr, pr_out, out_sem.at[0])]
    for k in (1, F - 1, *range(2, F - 1)):
        copy = push(dg.at[f], dg.at[f], d_send.at[k], d_recv.at[k], {"fs": fs_at(k)})
        copy.start()
        sends.append(copy)
    for k in (1, F - 1, *range(2, F - 1)):
        push(dg.at[f], dg.at[fs_at(-k)], d_send.at[k], d_recv.at[k], {"fs": fs_at(-k)}).wait_recv()
    gathered = dg[...].astype(jnp.float32)
    for p in range(2):
        d[p] = jnp.concatenate(
            [gathered[q, p * ranks : (p + 1) * ranks] for q in range(F)], axis=0
        ).T.astype(jnp.bfloat16)
    outs.append(fetch(d, d_out, out_sem.at[1]))

    for p in range(2):
        squares = jnp.zeros((d.shape[1], LANES), jnp.float32)
        update = jnp.dot(d[p], b[p], preferred_element_type=jnp.float32)
        for at in range(0, update.shape[1], LANES):
            part = update[:, at : at + LANES]
            squares = squares + part * part
        ss[t, p] = jnp.full((8, LANES), jnp.sum(squares), jnp.float32)
    for k in range(1, T):
        copy = push(ss.at[t], ss.at[t], n_send.at[k], n_recv.at[k], {"tp": tp_at(k)})
        copy.start()
        sends.append(copy)
    for k in range(1, T):
        push(ss.at[t], ss.at[tp_at(-k)], n_send.at[k], n_recv.at[k], {"tp": tp_at(-k)}).wait_recv()
    outs.append(fetch(ss, ss_out, out_sem.at[2]))

    outs.append(fetch(wg.at[f], wg_out.at[f], wo_sem.at[0]))
    push(wg.at[f, 1], wg.at[left, 1], w_send.at[1], w_recv.at[1], {"fs": left}).wait_recv()
    outs.append(fetch(wg.at[left], wg_out.at[left], wo_sem.at[1]))
    push(wg.at[f, 0], wg.at[right, 0], wl_send.at[0], wl_recv.at[0], {"fs": right}).wait_recv()
    outs.append(fetch(wg.at[right], wg_out.at[right], wo_sem.at[2]))
    push(wg.at[left, 0], wg.at[far, 0], w_send.at[2], w_recv.at[2], {"fs": left}).wait_recv()
    push(wg.at[right, 1], wg.at[far, 1], wl_send.at[2], wl_recv.at[2], {"fs": right}).wait_recv()
    outs.append(fetch(wg.at[far], wg_out.at[far], wo_sem.at[3]))
    for copy in outs:
        copy.wait()
    for copy in sends:
        copy.wait_send()


def finish(
    F, entries,
    at_ref, pr, d, ss, wg, bf, bv, wf, wv, ff, fv, sf, sv,
    nff, nsf, stf, nwf, cof, nfv, nsv, stv, nwv, cov,
):
    f = at_ref[0]
    low = lax.broadcasted_iota(jnp.int32, (wg.shape[3], LANES), 1) < LANES // 2
    ranks = ff.shape[0]
    tiles = wg.shape[2] // 2
    cols = wf.shape[1]
    for p, (basis, weight, first, second, nf, ns, step, nw, copy) in enumerate(
        ((bf, wf, ff, sf, nff, nsf, stf, nwf, cof), (bv, wv, fv, sv, nfv, nsv, stv, nwv, cov))
    ):
        @pl.when(pl.program_id(0) == 0)
        def _():
            nf[...], ns[...] = new_moments(pr[p * ranks : (p + 1) * ranks], first[...], second[...])

        square = ss[0, p, 0:1, 0:1]
        for q in range(1, ss.shape[0]):
            square = square + ss[q, p, 0:1, 0:1]
        scale = 1.0 / jnp.sqrt(square / entries + epsilon)
        steps = jnp.dot(d[p], basis[...], preferred_element_type=jnp.float32) * scale
        own = steps[:, :cols]
        for q in range(1, F):
            own = jnp.where(f == q, steps[:, q * cols : (q + 1) * cols], own)
        step[...] = own
        nw[...] = weight[...] - rate * own
        parts = []
        for q in range(0, F, 2):
            parts += [wg[q, 0, p * tiles + i].astype(jnp.float32) for i in range(tiles)]
            even = wg[q, 0, 2 * tiles].astype(jnp.float32)
            odd = wg[q + 1, 0, 2 * tiles].astype(jnp.float32)
            if p == 0:
                parts.append(jnp.where(low, even, odd))
            else:
                parts.append(pltpu.roll(jnp.where(low, odd, even), LANES // 2, 1))
            parts += [wg[q + 1, 0, p * tiles + i].astype(jnp.float32) for i in range(tiles)]
        for i, part in enumerate(parts):
            at = i * LANES
            copy[:, at : at + LANES] = (part - rate * steps[:, at : at + LANES]).astype(jnp.bfloat16)


def kernel_body(
    F, T,
    saved_input, cot_forget, cot_value, basis_forget, basis_value,
    first_forget, first_value, second_forget, second_value, weight_forget, weight_value,
):
    tokens, cols = saved_input.shape
    width, rank = basis_forget.shape
    ranks = first_forget.shape[0]
    rows = weight_forget.shape[0]
    block = tokens // T
    tiles = 2 * (rows // LANES) + 1
    half = cols // 2
    f32, bf16 = jnp.float32, jnp.bfloat16
    DMA = pltpu.SemaphoreType.DMA
    VMEM = pltpu.VMEM
    anywhere = pl.BlockSpec(memory_space=pl.ANY)
    in_hbm = pl.BlockSpec(memory_space=pltpu.HBM)
    bases = (basis_forget.T, basis_value.T)
    weights = (weight_forget.T, weight_value.T)
    moments_in = (first_forget, first_value, second_forget, second_value)

    projected, direction, squares, gathered = pl.pallas_call(
        functools.partial(exchange, F, T),
        out_shape=(
            jax.ShapeDtypeStruct((2 * ranks, cols), f32),
            jax.ShapeDtypeStruct((2, cols, rank), bf16),
            jax.ShapeDtypeStruct((T, 2, 8, LANES), f32),
            jax.ShapeDtypeStruct((F, 2, tiles, half, LANES), bf16),
        ),
        in_specs=[in_hbm] * 11,
        out_specs=(anywhere,) * 4,
        scratch_shapes=[
            VMEM((cols, tokens), bf16),
            VMEM((2, cols, tokens), bf16),
            VMEM((2, rank, width), bf16),
            VMEM((2, ranks, cols), f32),
            VMEM((2, ranks, cols), f32),
            VMEM((2, cols, rows), f32),
            VMEM((T, cols, block), bf16),
            VMEM((2, rank, block), bf16),
            VMEM((T, 2, rank, block), bf16),
            VMEM((F, 2 * ranks, cols), bf16),
            VMEM((F, 2 * ranks, cols), bf16),
            VMEM((2 * ranks, cols), f32),
            VMEM((F, 2 * ranks, cols), bf16),
            VMEM((2, cols, rank), bf16),
            VMEM((T, 2, 8, LANES), f32),
            VMEM((F, 2, tiles, half, LANES), bf16),
            DMA((11,)), DMA, DMA((T,)), DMA((T,)), DMA((T,)), DMA((T,)), DMA((T,)), DMA((T,)),
            DMA((F,)), DMA((F,)), DMA((F,)), DMA((F,)), DMA((T,)), DMA((T,)),
            DMA((3,)), DMA((3,)), DMA((3,)), DMA((3,)), DMA((3,)), DMA((4,)),
        ],
        compiler_params=pltpu.CompilerParams(
            collective_id=0, has_side_effects=True, vmem_limit_bytes=63 * 2**20
        ),
        name="exchange",
    )(saved_input.T, cot_forget.T, cot_value.T, *bases, *moments_in, *weights)

    blocks = 3
    deep = half // blocks
    entries = float(width * cols * T)

    def const(*shape):
        return pl.BlockSpec(shape, lambda j, at: (0,) * len(shape))

    def rows_of(count):
        return pl.BlockSpec((deep, count), lambda j, at: (j, 0))

    one_out = [
        jax.ShapeDtypeStruct((ranks, cols), f32), jax.ShapeDtypeStruct((ranks, cols), f32),
        jax.ShapeDtypeStruct((cols, rows), f32), jax.ShapeDtypeStruct((cols, rows), f32),
        jax.ShapeDtypeStruct((cols, width), bf16),
    ]
    one_spec = [const(ranks, cols), const(ranks, cols), rows_of(rows), rows_of(rows), rows_of(width)]
    results = pl.pallas_call(
        functools.partial(finish, F, entries),
        out_shape=one_out * 2,
        grid_spec=pltpu.PrefetchScalarGridSpec(
            num_scalar_prefetch=1,
            grid=(2 * blocks,),
            in_specs=[
                const(2 * ranks, cols),
                pl.BlockSpec((2, deep, rank), lambda j, at: (0, j, 0)),
                const(T, 2, 8, LANES),
                pl.BlockSpec((F, 1, tiles, deep, LANES), lambda j, at: (0, j // blocks, 0, j % blocks, 0)),
                const(rank, width), const(rank, width), rows_of(rows), rows_of(rows),
                *([const(ranks, cols)] * 4),
            ],
            out_specs=one_spec * 2,
        ),
        compiler_params=pltpu.CompilerParams(
            dimension_semantics=("arbitrary",), vmem_limit_bytes=32 * 2**20
        ),
        name="finish",
    )(lax.axis_index("fs").reshape(1), projected, direction, squares, gathered, *bases, *weights, *moments_in)
    return tuple(r if i % 5 < 2 else r.T for i, r in enumerate(results))


def program(F, T, *args):
    tokens, cols = args[0].shape
    ranks = args[5].shape[0]
    rows = args[9].shape[0]
    block_fits = tokens == T * LANES and cols % 96 == 0 and ranks % 8 == 0
    rows_fit = rows > LANES and rows % LANES == LANES // 2
    if F == 4 and T % 2 == 0 and block_fits and rows_fit:
        return kernel_body(F, T, *args)
    return body(*args)


def solution(mesh):
    split = P("fs", "tp")
    in_specs = (split, split, split, P(), P()) + (split,) * 6
    out_specs = (split, split, split, split, P(None, "tp")) * 2
    inner = functools.partial(program, mesh.shape["fs"], mesh.shape["tp"])
    return jax.shard_map(inner, mesh=mesh, in_specs=in_specs, out_specs=out_specs, check_vma=False)
```

```python
import functools

import jax
import jax.numpy as jnp
from jax import lax
from jax.experimental import pallas as pl
from jax.experimental.pallas import tpu as pltpu
from jax.sharding import PartitionSpec as P

MESH = pl.DeviceIdType.MESH
LANES = 128

beta_one = 0.8
beta_two = 0.9
rate = 0.02
epsilon = 1e-06


def contract(left_part, right_part):
    return lax.dot_general(
        left_part,
        right_part,
        (((0,), (0,)), ((), ())),
        precision=lax.Precision.HIGHEST,
        preferred_element_type=jnp.float32,
    )


def moments(projected, first, second):
    new_first = beta_one * first + (1.0 - beta_one) * projected
    new_second = beta_two * second + (1.0 - beta_two) * projected * projected
    direction = (new_first / jnp.sqrt(new_second)).astype(jnp.bfloat16)
    return (new_first, new_second, direction)


def body(
    saved_input,
    cot_forget,
    cot_value,
    basis_forget,
    basis_value,
    first_forget,
    first_value,
    second_forget,
    second_value,
    weight_forget,
    weight_value,
):
    col_width = cot_forget.shape[1]
    own_rows = weight_forget.shape[0]
    col_first = lax.axis_index("tp") * col_width
    row_start = lax.axis_index("fs") * own_rows
    rows_forget = lax.dynamic_slice_in_dim(basis_forget, row_start, own_rows, 0)
    rows_value = lax.dynamic_slice_in_dim(basis_value, row_start, own_rows, 0)
    both_cots = jnp.concatenate([cot_forget, cot_value], axis=1)
    cols_forget = lax.dynamic_slice_in_dim(basis_forget, col_first, col_width, 0)
    cols_value = lax.dynamic_slice_in_dim(basis_value, col_first, col_width, 0)
    partial_forget = jnp.dot(saved_input, cols_forget, preferred_element_type=jnp.float32)
    partial_value = jnp.dot(saved_input, cols_value, preferred_element_type=jnp.float32)
    summed_forget, summed_value = lax.psum((partial_forget, partial_value), "tp")
    cots_wide = both_cots.astype(jnp.float32)
    projected = lax.psum_scatter(
        jnp.concatenate(
            [
                contract(summed_forget, cots_wide[:, :col_width]),
                contract(summed_value, cots_wide[:, col_width:]),
            ],
            axis=1,
        ),
        "fs",
        scatter_dimension=0,
        tiled=True,
    )
    new_first_forget, new_second_forget, direction_forget = moments(
        projected[:, :col_width], first_forget, second_forget
    )
    new_first_value, new_second_value, direction_value = moments(
        projected[:, col_width:], first_value, second_value
    )
    update_forget = jnp.dot(
        rows_forget,
        lax.all_gather(direction_forget, "fs", axis=0, tiled=True),
        preferred_element_type=jnp.float32,
    )
    update_value = jnp.dot(
        rows_value,
        lax.all_gather(direction_value, "fs", axis=0, tiled=True),
        preferred_element_type=jnp.float32,
    )
    square_forget, square_value = lax.psum(
        (jnp.sum(update_forget * update_forget), jnp.sum(update_value * update_value)), ("fs", "tp")
    )
    entries = float(basis_forget.shape[0] * weight_forget.shape[1] * lax.axis_size("tp"))
    step_forget = update_forget / jnp.sqrt(square_forget / entries + epsilon)
    step_value = update_value / jnp.sqrt(square_value / entries + epsilon)
    new_weight_forget = weight_forget - rate * step_forget
    new_weight_value = weight_value - rate * step_value
    copy_forget, copy_value = (
        lax.all_gather(new_weight_forget.astype(jnp.bfloat16), "fs", axis=0, tiled=True),
        lax.all_gather(new_weight_value.astype(jnp.bfloat16), "fs", axis=0, tiled=True),
    )
    return (
        new_first_forget,
        new_second_forget,
        step_forget,
        new_weight_forget,
        copy_forget,
        new_first_value,
        new_second_value,
        step_value,
        new_weight_value,
        copy_value,
    )


def pack(weights, odd, half):
    deep = weights[0].shape[0] // 2
    cols = weights[0].shape[1]
    side = LANES // 2
    whole = cols - side
    tiles = []
    rests = []
    for weight in weights:
        rows = weight[deep * half : deep * (half + 1)]
        kept = jnp.where(odd, rows[:, side:], rows[:, :whole])
        tiles += [kept[:, at : at + LANES] for at in range(0, whole, LANES)]
        rests.append(jnp.where(odd, rows[:, :side], rows[:, whole:]))
    rest = jnp.where(
        odd,
        jnp.concatenate([rests[1], rests[0]], axis=1),
        jnp.concatenate(rests, axis=1),
    )
    return jnp.stack(tiles + [rest]).astype(jnp.bfloat16)


def new_moments(projected, first, second):
    new_first = beta_one * first + (1.0 - beta_one) * projected
    new_second = beta_two * second + (1.0 - beta_two) * projected * projected
    return new_first, new_second


def contract_tokens(left, right):
    return lax.dot_general(
        left, right, (((1,), (1,)), ((), ())), preferred_element_type=jnp.float32
    )


def exchange(
    F, T,
    s_hbm, cf_hbm, cv_hbm, bf_hbm, bv_hbm, ff_hbm, fv_hbm, sf_hbm, sv_hbm, wf_hbm, wv_hbm,
    pr_out, d_out, ss_out, wg_out,
    s, c, b, fm, sm, w, sg, z, zg, psend, prx, pr, dg, d, ss, wg,
    in_sem, sg_own, sg_send, sg_recv, z_send, z_recv, zf_send, zf_recv,
    p_send, p_recv, d_send, d_recv, n_send, n_recv, w_send, w_recv, out_sem, own_out, wo_sem,
):
    f = lax.axis_index("fs")
    t = lax.axis_index("tp")
    ranks = psend.shape[1] // 2
    block = zg.shape[3]
    pair = t + 1 - 2 * lax.rem(t, 2)

    def tp_at(k):
        return lax.rem(t + k + T, T)

    def fs_at(k):
        return lax.rem(f + k + F, F)

    def tokens(k):
        return pl.ds(pl.multiple_of(k * block, block), block)

    def fetch(src, dst, sem):
        copy = pltpu.make_async_copy(src, dst, sem)
        copy.start()
        return copy

    def push(src, dst, send, recv, where):
        return pltpu.make_async_remote_copy(
            src_ref=src, dst_ref=dst, send_sem=send, recv_sem=recv,
            device_id=where, device_id_type=MESH,
        )

    load_w = [fetch(wf_hbm, w.at[0], in_sem.at[0]), fetch(wv_hbm, w.at[1], in_sem.at[1])]
    load_s = fetch(s_hbm, s, in_sem.at[2])
    load_own = fetch(s_hbm.at[:, tokens(t)], sg.at[t], sg_own)
    load_b = [fetch(bf_hbm, b.at[0], in_sem.at[3]), fetch(bv_hbm, b.at[1], in_sem.at[4])]
    load_c = [fetch(cf_hbm, c.at[0], in_sem.at[5]), fetch(cv_hbm, c.at[1], in_sem.at[6])]
    load_m = [
        fetch(ff_hbm, fm.at[0], in_sem.at[7]), fetch(fv_hbm, fm.at[1], in_sem.at[8]),
        fetch(sf_hbm, sm.at[0], in_sem.at[9]), fetch(sv_hbm, sm.at[1], in_sem.at[10]),
    ]

    barrier = pltpu.get_barrier_semaphore()
    for k in range(1, T):
        pl.semaphore_signal(barrier, inc=1, device_id={"tp": tp_at(k)}, device_id_type=MESH)
    for k in range(1, F):
        pl.semaphore_signal(barrier, inc=1, device_id={"fs": fs_at(k)}, device_id_type=MESH)
    for p in range(2):
        load_w[p].wait()
    both = [w[0], w[1]]
    for half in range(2):
        wg[f, half] = pack(both, lax.rem(f, 2) == 1, half)
    load_s.wait()
    pl.semaphore_wait(barrier, T + F - 2)

    sends = []
    for k in range(1, T):
        copy = push(s.at[:, tokens(tp_at(k))], sg.at[t], sg_send.at[k], sg_recv.at[k], {"tp": tp_at(k)})
        copy.start()
        sends.append(copy)
    def travel(k, half, way):
        block = fs_at(-k) if way == 0 else fs_at(k)
        return push(
            wg.at[block, half], wg.at[block, half],
            w_send.at[way, k, half], w_recv.at[way, k, half], {"fs": fs_at(1 if way == 0 else -1)},
        )

    def passes_on(k, way):
        place = f if way == 0 else F - 1 - f
        return jnp.logical_and(place >= k, place < F - 1)

    def comes_in(k, way):
        place = f if way == 0 else F - 1 - f
        return place >= k

    def leave(k, half, way):
        block = fs_at(-k) if way == 0 else fs_at(k)
        return pltpu.make_async_copy(wg.at[block, half], wg_out.at[block, half], wo_sem.at[way, k - 1, half])

    def relay(k, half):
        for way in range(2):
            @pl.when(comes_in(k, way))
            def _():
                block = fs_at(-k) if way == 0 else fs_at(k)
                push(
                    wg.at[f, half], wg.at[block, half],
                    w_send.at[way, k - 1, half], w_recv.at[way, k - 1, half],
                    {"fs": fs_at(-1 if way == 0 else 1)},
                ).wait_recv()

                if k < F - 1:
                    @pl.when(passes_on(k, way))
                    def _():
                        travel(k, half, way).start()

                leave(k, half, way).start()

    for half in range(2):
        for way in range(2):
            @pl.when(passes_on(0, way))
            def _():
                travel(0, half, way).start()
    outs = [fetch(wg.at[f], wg_out.at[f], own_out)]

    load_own.wait()
    for copy in load_b:
        copy.wait()
    for k in range(1, T):
        source = tp_at(-k)
        push(s.at[:, tokens(t)], sg.at[source], sg_send.at[k], sg_recv.at[k], {"tp": source}).wait_recv()
    inputs = sg[...].reshape(b.shape[2], block)
    for p in range(2):
        z[p] = jnp.dot(b[p], inputs, preferred_element_type=jnp.float32).astype(jnp.bfloat16)

    chips = T // 2
    to_pair = push(z, zg.at[t], zf_send.at[0], zf_recv.at[0], {"tp": pair})
    for k in range(1, chips):
        copy = push(z, zg.at[t], z_send.at[k], z_recv.at[k], {"tp": tp_at(2 * k)})
        copy.start()
        sends.append(copy)
    to_pair.start()
    sends.append(to_pair)
    relay(1, 0)

    for copy in load_c:
        copy.wait()
    partial = [contract_tokens(z[p], c[p, :, tokens(t)]) for p in range(2)]

    def add(partial, source):
        return [
            partial[p] + contract_tokens(zg[source, p], c[p, :, tokens(source)])
            for p in range(2)
        ]

    push(z, zg.at[pair], zf_send.at[0], zf_recv.at[0], {"tp": pair}).wait_recv()
    partial = add(partial, pair)
    for k in range(1, chips):
        source = tp_at(-2 * k)
        push(z, zg.at[source], z_send.at[k], z_recv.at[k], {"tp": source}).wait_recv()
        copy = push(zg.at[source], zg.at[source], zf_send.at[k], zf_recv.at[k], {"tp": pair})
        copy.start()
        sends.append(copy)
        partial = add(partial, source)
        if k == chips - 1:
            relay(1, 1)
    for k in range(1, chips):
        source = lax.rem(pair - 2 * k + T, T)
        push(z, zg.at[source], zf_send.at[k], zf_recv.at[k], {"tp": pair}).wait_recv()
        partial = add(partial, source)

    for q in range(F):
        rows = jnp.concatenate([part[q * ranks : (q + 1) * ranks] for part in partial], axis=0)
        psend[q] = rows.astype(jnp.bfloat16)
        own = jnp.where(f == q, rows, 0.0)
        total = own if q == 0 else total + own
    for k in (1, F - 1, *range(2, F - 1)):
        copy = push(psend.at[fs_at(k)], prx.at[f], p_send.at[k], p_recv.at[k], {"fs": fs_at(k)})
        copy.start()
        sends.append(copy)

    relay(2, 0)
    for copy in load_m:
        copy.wait()
    for k in (1, F - 1, *range(2, F - 1)):
        push(psend.at[f], prx.at[fs_at(-k)], p_send.at[k], p_recv.at[k], {"fs": fs_at(-k)}).wait_recv()
    for k in range(1, F):
        total = total + prx[fs_at(-k)].astype(jnp.float32)
    pr[...] = total
    new_first, new_second = new_moments(total, fm[...].reshape(total.shape), sm[...].reshape(total.shape))
    dg[f] = (new_first / jnp.sqrt(new_second)).astype(jnp.bfloat16)
    outs.append(fetch(pr, pr_out, out_sem.at[0]))
    for k in (1, F - 1, *range(2, F - 1)):
        copy = push(dg.at[f], dg.at[f], d_send.at[k], d_recv.at[k], {"fs": fs_at(k)})
        copy.start()
        sends.append(copy)
    relay(2, 1)
    for k in (1, F - 1, *range(2, F - 1)):
        push(dg.at[f], dg.at[fs_at(-k)], d_send.at[k], d_recv.at[k], {"fs": fs_at(-k)}).wait_recv()
    gathered = dg[...].astype(jnp.float32)
    for p in range(2):
        d[p] = jnp.concatenate(
            [gathered[q, p * ranks : (p + 1) * ranks] for q in range(F)], axis=0
        ).T.astype(jnp.bfloat16)
    outs.append(fetch(d, d_out, out_sem.at[1]))

    for p in range(2):
        squares = jnp.zeros((d.shape[1], LANES), jnp.float32)
        update = jnp.dot(d[p], b[p], preferred_element_type=jnp.float32)
        for at in range(0, update.shape[1], LANES):
            part = update[:, at : at + LANES]
            squares = squares + part * part
        ss[t, p] = jnp.full((8, LANES), jnp.sum(squares), jnp.float32)
    for k in range(1, T):
        copy = push(ss.at[t], ss.at[t], n_send.at[k], n_recv.at[k], {"tp": tp_at(k)})
        copy.start()
        sends.append(copy)
    for k in range(1, T):
        push(ss.at[t], ss.at[tp_at(-k)], n_send.at[k], n_recv.at[k], {"tp": tp_at(-k)}).wait_recv()
    outs.append(fetch(ss, ss_out, out_sem.at[2]))

    for k in range(3, F):
        for half in range(2):
            relay(k, half)
    for half in range(2):
        for way in range(2):
            for k in range(F - 1):
                @pl.when(passes_on(k, way))
                def _():
                    travel(k, half, way).wait_send()
            for k in range(1, F):
                @pl.when(comes_in(k, way))
                def _():
                    leave(k, half, way).wait()
    for copy in outs:
        copy.wait()
    for copy in sends:
        copy.wait_send()


def finish(
    F, entries,
    at_ref, pr, d, ss, wg, bf, bv, wf, wv, ff, fv, sf, sv,
    nff, nsf, stf, nwf, cof, nfv, nsv, stv, nwv, cov,
):
    f = at_ref[0]
    low = lax.broadcasted_iota(jnp.int32, (wg.shape[3], LANES), 1) < LANES // 2
    ranks = ff.shape[0]
    tiles = wg.shape[2] // 2
    cols = wf.shape[1]
    for p, (basis, weight, first, second, nf, ns, step, nw, copy) in enumerate(
        ((bf, wf, ff, sf, nff, nsf, stf, nwf, cof), (bv, wv, fv, sv, nfv, nsv, stv, nwv, cov))
    ):
        @pl.when(pl.program_id(0) == 0)
        def _():
            nf[...], ns[...] = new_moments(pr[p * ranks : (p + 1) * ranks], first[...], second[...])

        square = ss[0, p, 0:1, 0:1]
        for q in range(1, ss.shape[0]):
            square = square + ss[q, p, 0:1, 0:1]
        scale = 1.0 / jnp.sqrt(square / entries + epsilon)
        steps = jnp.dot(d[p], basis[...], preferred_element_type=jnp.float32) * scale
        own = steps[:, :cols]
        for q in range(1, F):
            own = jnp.where(f == q, steps[:, q * cols : (q + 1) * cols], own)
        step[...] = own
        nw[...] = weight[...] - rate * own
        parts = []
        for q in range(0, F, 2):
            parts += [wg[q, 0, p * tiles + i].astype(jnp.float32) for i in range(tiles)]
            even = wg[q, 0, 2 * tiles].astype(jnp.float32)
            odd = wg[q + 1, 0, 2 * tiles].astype(jnp.float32)
            if p == 0:
                parts.append(jnp.where(low, even, odd))
            else:
                parts.append(pltpu.roll(jnp.where(low, odd, even), LANES // 2, 1))
            parts += [wg[q + 1, 0, p * tiles + i].astype(jnp.float32) for i in range(tiles)]
        for i, part in enumerate(parts):
            at = i * LANES
            copy[:, at : at + LANES] = (part - rate * steps[:, at : at + LANES]).astype(jnp.bfloat16)


def kernel_body(
    F, T,
    saved_input, cot_forget, cot_value, basis_forget, basis_value,
    first_forget, first_value, second_forget, second_value, weight_forget, weight_value,
):
    tokens, cols = saved_input.shape
    width, rank = basis_forget.shape
    ranks = first_forget.shape[0]
    rows = weight_forget.shape[0]
    block = tokens // T
    tiles = 2 * (rows // LANES) + 1
    half = cols // 2
    f32, bf16 = jnp.float32, jnp.bfloat16
    DMA = pltpu.SemaphoreType.DMA
    VMEM = pltpu.VMEM
    anywhere = pl.BlockSpec(memory_space=pl.ANY)
    in_hbm = pl.BlockSpec(memory_space=pltpu.HBM)
    bases = (basis_forget.T, basis_value.T)
    weights = (weight_forget.T, weight_value.T)
    moments_in = (first_forget, first_value, second_forget, second_value)

    projected, direction, squares, gathered = pl.pallas_call(
        functools.partial(exchange, F, T),
        out_shape=(
            jax.ShapeDtypeStruct((2 * ranks, cols), f32),
            jax.ShapeDtypeStruct((2, cols, rank), bf16),
            jax.ShapeDtypeStruct((T, 2, 8, LANES), f32),
            jax.ShapeDtypeStruct((F, 2, tiles, half, LANES), bf16),
        ),
        in_specs=[in_hbm] * 11,
        out_specs=(anywhere,) * 4,
        scratch_shapes=[
            VMEM((cols, tokens), bf16),
            VMEM((2, cols, tokens), bf16),
            VMEM((2, rank, width), bf16),
            VMEM((2, ranks, cols), f32),
            VMEM((2, ranks, cols), f32),
            VMEM((2, cols, rows), f32),
            VMEM((T, cols, block), bf16),
            VMEM((2, rank, block), bf16),
            VMEM((T, 2, rank, block), bf16),
            VMEM((F, 2 * ranks, cols), bf16),
            VMEM((F, 2 * ranks, cols), bf16),
            VMEM((2 * ranks, cols), f32),
            VMEM((F, 2 * ranks, cols), bf16),
            VMEM((2, cols, rank), bf16),
            VMEM((T, 2, 8, LANES), f32),
            VMEM((F, 2, tiles, half, LANES), bf16),
            DMA((11,)), DMA, DMA((T,)), DMA((T,)), DMA((T,)), DMA((T,)), DMA((T,)), DMA((T,)),
            DMA((F,)), DMA((F,)), DMA((F,)), DMA((F,)), DMA((T,)), DMA((T,)),
            DMA((2, F - 1, 2)), DMA((2, F - 1, 2)), DMA((3,)), DMA, DMA((2, F - 1, 2)),
        ],
        compiler_params=pltpu.CompilerParams(
            collective_id=0, has_side_effects=True, vmem_limit_bytes=63 * 2**20
        ),
        name="exchange",
    )(saved_input.T, cot_forget.T, cot_value.T, *bases, *moments_in, *weights)

    blocks = 3
    deep = half // blocks
    entries = float(width * cols * T)

    def const(*shape):
        return pl.BlockSpec(shape, lambda j, at: (0,) * len(shape))

    def rows_of(count):
        return pl.BlockSpec((deep, count), lambda j, at: (j, 0))

    one_out = [
        jax.ShapeDtypeStruct((ranks, cols), f32), jax.ShapeDtypeStruct((ranks, cols), f32),
        jax.ShapeDtypeStruct((cols, rows), f32), jax.ShapeDtypeStruct((cols, rows), f32),
        jax.ShapeDtypeStruct((cols, width), bf16),
    ]
    one_spec = [const(ranks, cols), const(ranks, cols), rows_of(rows), rows_of(rows), rows_of(width)]
    results = pl.pallas_call(
        functools.partial(finish, F, entries),
        out_shape=one_out * 2,
        grid_spec=pltpu.PrefetchScalarGridSpec(
            num_scalar_prefetch=1,
            grid=(2 * blocks,),
            in_specs=[
                const(2 * ranks, cols),
                pl.BlockSpec((2, deep, rank), lambda j, at: (0, j, 0)),
                const(T, 2, 8, LANES),
                pl.BlockSpec((F, 1, tiles, deep, LANES), lambda j, at: (0, j // blocks, 0, j % blocks, 0)),
                const(rank, width), const(rank, width), rows_of(rows), rows_of(rows),
                *([const(ranks, cols)] * 4),
            ],
            out_specs=one_spec * 2,
        ),
        compiler_params=pltpu.CompilerParams(
            dimension_semantics=("arbitrary",), vmem_limit_bytes=63 * 2**20
        ),
        name="finish",
    )(lax.axis_index("fs").reshape(1), projected, direction, squares, gathered, *bases, *weights, *moments_in)
    return tuple(r if i % 5 < 2 else r.T for i, r in enumerate(results))


def program(F, T, *args):
    tokens, cols = args[0].shape
    ranks = args[5].shape[0]
    rows = args[9].shape[0]
    block_fits = tokens == T * LANES and cols % 96 == 0 and ranks % 8 == 0
    rows_fit = rows > LANES and rows % LANES == LANES // 2
    if F == 4 and T % 2 == 0 and block_fits and rows_fit:
        return kernel_body(F, T, *args)
    return body(*args)


def solution(mesh):
    split = P("fs", "tp")
    in_specs = (split, split, split, P(), P()) + (split,) * 6
    out_specs = (split, split, split, split, P(None, "tp")) * 2
    inner = functools.partial(program, mesh.shape["fs"], mesh.shape["tp"])
    return jax.shard_map(inner, mesh=mesh, in_specs=in_specs, out_specs=out_specs, check_vma=False)
```
